32 devices in a mesh: fs: 8 (over z, y), tp: 4 (over x, core).
Axes of the slice: x: 2, y: 2, z: 4, core: 2. Of those that a mesh axis runs over, the one named last changes fastest.
Arguments:
- x_next: bfloat16 [1536, 2048], P(('fs', 'tp')), may hold values from -6 to 6
- x_prev: bfloat16 [1536, 2048], P(('fs', 'tp')), may hold values from -6 to 6
- grad_out: bfloat16 [1536, 2048], P(('fs', 'tp')), may hold values from -6 to 6
- gate_w: bfloat16 [2048, 2816], P('fs', 'tp'), may hold values from -0.125 to 0.125
- up_w: bfloat16 [2048, 2816], P('fs', 'tp'), may hold values from -0.125 to 0.125
- down_w: bfloat16 [2816, 2048], P('tp', 'fs'), may hold values from -0.109375 to 0.109375
- acc_gate: float32 [2048, 2816], P('fs', 'tp'), may hold values from -2.5 to 2.5
- acc_up: float32 [2048, 2816], P('fs', 'tp'), may hold values from -2.5 to 2.5
- acc_down: float32 [2816, 2048], P('tp', 'fs'), may hold values from -2.5 to 2.5
Outputs:
- out_next: bfloat16 [1536, 2048], P(('fs', 'tp'))
- saved_hidden: bfloat16 [1536, 2816], P('fs', 'tp')
- grad_input: bfloat16 [1536, 2048], P(('fs', 'tp'))
- new_gate: float32 [2048, 2816], P('fs', 'tp')
- new_up: float32 [2048, 2816], P('fs', 'tp')
- new_down: float32 [2816, 2048], P('tp', 'fs')
The draws below stay inside these ranges and needn't reach their ends.
All inputs are finite; a program needn't handle non-finite values.
Results may differ from the reference program's by a relative error of at most 0.014.
Values may be sent and summed in bfloat16 or wider, within the bound.
A program may use at most 64 MiB of HBM per device.

```python
import math
import jax
import jax.numpy as jnp
from jax import lax

D = 2048
FF = 2816
TOKENS = 1536
N_TP = 4


def spiked(drawn, rng, source, target, shards_of, factor):
    owner, partner = [(jnp.arange(drawn.shape[dim]) // (drawn.shape[dim] // shards_of)).reshape([-1 if axis == dim else 1 for axis in range(drawn.ndim)]) for dim in (source, target)]
    chosen = jax.random.permutation(rng, shards_of)[partner]
    strong = (owner == chosen) | (owner == (partner + shards_of // 2) % shards_of)
    return jnp.where(strong, factor * drawn, drawn)


def block_scale(key, extent, pieces, smallest, top_value):
    def one(axis_at, shards_of):
        draws = jax.random.uniform(jax.random.fold_in(jax.random.fold_in(key, 6), axis_at), (shards_of,), jnp.float32, smallest / len(pieces), top_value / len(pieces))
        return jnp.repeat(jnp.exp(draws), extent[axis_at] // shards_of).reshape((-1,) + (1,) * (len(extent) - axis_at - 1))

    loudness = one(*pieces[0])
    for cut in pieces[1:]:
        loudness = loudness * one(*cut)
    return loudness


def centred(own_key, dims, spread, bound, pieces=(), dtype=jnp.bfloat16):
    level = block_scale(own_key, dims, pieces, -0.22, 0.18) if pieces else 1.0
    entries = jax.random.normal(own_key, dims, jnp.float32) * spread * level
    return jnp.minimum(jnp.maximum(entries, -bound), bound).astype(dtype)


def heavy_noise(rng, shape, spread, limit, pieces, heavy, kind=jnp.bfloat16):
    entries = spread * jax.random.normal(rng, shape, jnp.float32)
    if pieces:
        entries = entries * block_scale(rng, shape, pieces, -0.22, 0.18)
    return jnp.clip(spiked(entries, jax.random.fold_in(rng, 3), *heavy), -limit, limit).astype(kind)


def setup_inputs(seed: int = 0) -> dict:
    key_list = jax.random.split(jax.random.key(seed), 10)
    return {
        "x_next": centred(key_list[0], (TOKENS, D), 1.0, 6.0, ((0, 32),)),
        "x_prev": centred(key_list[1], (TOKENS, D), 1.0, 6.0, ((0, 32),)),
        "grad_out": heavy_noise(key_list[2], (TOKENS, D), 1.0, 6.0, ((0, 32),), (0, 1, 32, 2.75)),
        "gate_w": centred(key_list[3], (D, FF), D ** -0.5, 0.125, ((0, 8), (1, 4))),
        "up_w": centred(key_list[4], (D, FF), D ** -0.5, 0.125, ((0, 8), (1, 4))),
        "down_w": centred(key_list[5], (FF, D), FF ** -0.5, 0.109375, ((0, 4), (1, 8))),
        "acc_gate": centred(key_list[6], (D, FF), 0.3, 2.5, ((0, 8), (1, 4)), jnp.float32),
        "acc_up": centred(key_list[7], (D, FF), 0.3, 2.5, ((0, 8), (1, 4)), jnp.float32),
        "acc_down": centred(key_list[8], (FF, D), 0.3, 2.5, ((0, 4), (1, 8)), jnp.float32),
    }


def block_sum(make_part):
    block = FF // N_TP
    total = None
    for index in range(N_TP):
        part = make_part(index * block, block)
        rounded = lax.optimization_barrier(part.astype(jnp.bfloat16)).astype(jnp.float32)
        total = rounded if total is None else total + rounded
    return total

def reference(x_next, x_prev, grad_out, gate_w, up_w, down_w, acc_gate, acc_up, acc_down):
    gate_next = jnp.dot(x_next, gate_w, preferred_element_type=jnp.float32)
    up_next = jnp.dot(x_next, up_w, preferred_element_type=jnp.float32)
    saved_hidden = (jax.nn.silu(gate_next) * up_next).astype(jnp.bfloat16)

    def out_part(start, width):
        return jnp.dot(saved_hidden[:, start:start + width], down_w[start:start + width], preferred_element_type=jnp.float32)
    out_next = block_sum(out_part).astype(jnp.bfloat16)
    gate_prev = jnp.dot(x_prev, gate_w, preferred_element_type=jnp.float32)
    up_prev = jnp.dot(x_prev, up_w, preferred_element_type=jnp.float32)
    grad_hidden = jnp.dot(grad_out, down_w.T, preferred_element_type=jnp.float32)
    sigmoid_gate = jax.nn.sigmoid(gate_prev)
    silu_gate = gate_prev * sigmoid_gate
    grad_gate = (grad_hidden * up_prev * sigmoid_gate * (1.0 + gate_prev * (1.0 - sigmoid_gate))).astype(jnp.bfloat16)
    grad_up = (grad_hidden * silu_gate).astype(jnp.bfloat16)
    hidden_prev = (silu_gate * up_prev).astype(jnp.bfloat16)

    def input_part(start, width):
        first = jnp.dot(grad_gate[:, start:start + width], gate_w[:, start:start + width].T, preferred_element_type=jnp.float32)
        second = jnp.dot(grad_up[:, start:start + width], up_w[:, start:start + width].T, preferred_element_type=jnp.float32)
        return first + second
    grad_input = block_sum(input_part).astype(jnp.bfloat16)
    factor = 1.0 / math.sqrt(TOKENS)
    new_gate = acc_gate + factor * jnp.dot(x_prev.T, grad_gate, preferred_element_type=jnp.float32)
    new_up = acc_up + factor * jnp.dot(x_prev.T, grad_up, preferred_element_type=jnp.float32)
    new_down = acc_down + factor * jnp.dot(hidden_prev.T, grad_out, preferred_element_type=jnp.float32)
    return (out_next, saved_hidden, grad_input, new_gate, new_up, new_down)
```

```python
import math

import jax
import jax.numpy as jnp
from jax import lax
from jax.experimental import pallas as pl
from jax.experimental.pallas import tpu as pltpu
from jax.sharding import PartitionSpec as P

MESH = pl.DeviceIdType.MESH
ANY = pl.BlockSpec(memory_space=pl.ANY)


def columns_of(size):
    side = 1
    while 8 * side * side <= size and size % (2 * side) == 0:
        side *= 2
    return side


def contract_rows(left, right):
    return lax.dot_general(
        left, right, (((0,), (0,)), ((), ())), preferred_element_type=jnp.float32
    )


def contract_cols(left, right):
    return lax.dot_general(
        left, right, (((1,), (1,)), ((), ())), preferred_element_type=jnp.float32
    )


def remote(source, target, send, recv, device):
    return pltpu.make_async_remote_copy(
        src_ref=source, dst_ref=target, send_sem=send, recv_sem=recv,
        device_id=device, device_id_type=MESH,
    )


class Spread:
    def __init__(self, fs, owns, fulls, send, recv):
        self.ny = columns_of(fs)
        self.nz = fs // self.ny
        self.fs, self.owns, self.fulls = fs, owns, fulls
        self.send, self.recv = send, recv
        self.f, self.t = lax.axis_index("fs"), lax.axis_index("tp")
        self.z, self.y = self.f // self.ny, lax.rem(self.f, self.ny)

    def flows(self, w, f, source, up, down, act):
        full = self.fulls[w].at[f]

        def go(kind, z, y):
            act(remote(source, full, self.send.at[w, kind, f], self.recv.at[w, f],
                       (z * self.ny + y, self.t)))

        if up:
            pl.when(self.z + 1 < self.nz)(lambda: go(0, self.z + 1, self.y))
        if down:
            pl.when(self.z > 0)(lambda: go(1, self.z - 1, self.y))
        for k in range(1, self.ny):
            go(1 + k, self.z, lax.rem(self.y + k, self.ny))

    def start(self):
        for w, own in enumerate(self.owns):
            self.flows(w, self.f, own, True, True, lambda c: c.start())

    def arrived(self, w, f):
        full = self.fulls[w].at[f]
        remote(full, full, self.send.at[w, 0, f], self.recv.at[w, f],
               (self.f, self.t)).wait_recv()

    def relay(self, act, wait):
        for d in range(1, self.nz):
            for w in range(len(self.owns)):
                def from_below(w=w, d=d):
                    f = (self.z - d) * self.ny + self.y
                    if wait:
                        self.arrived(w, f)
                    self.flows(w, f, self.fulls[w].at[f], True, False, act)

                def from_above(w=w, d=d):
                    f = (self.z + d) * self.ny + self.y
                    if wait:
                        self.arrived(w, f)
                    self.flows(w, f, self.fulls[w].at[f], False, True, act)

                pl.when(self.z >= d)(from_below)
                pl.when(self.z + d < self.nz)(from_above)

    def finish(self):
        for w in range(len(self.owns)):
            for z in range(self.nz):
                for k in range(1, self.ny):
                    self.arrived(w, z * self.ny + lax.rem(self.y + k, self.ny))
        for w, own in enumerate(self.owns):
            self.flows(w, self.f, own, True, True, lambda c: c.wait_send())
        self.relay(lambda c: c.wait_send(), False)


def stage_in(pairs, sem):
    copies = [pltpu.make_async_copy(a, b, sem.at[i]) for i, (a, b) in enumerate(pairs)]
    for copy in copies:
        copy.start()
    return copies


def gather_inputs(fs, tp, *refs):
    (gate, up, down, xn, xp, go, cols,
     gate_o, up_o, down_o, xn_o, xp_o, go_o, cols_o,
     *rest) = refs
    held, (wsend, wrecv, tsend, trecv, csend, crecv, dsend, drecv, lin, lout) = rest[:7], rest[7:]
    f, t = lax.axis_index("fs"), lax.axis_index("tp")
    sources = (gate, up, down, xn, xp, go, cols)
    into = stage_in(list(zip(sources, held)), lin)
    spread = Spread(fs, held[:3], (gate_o, up_o, down_o), wsend, wrecv)
    for copy in into[:3]:
        copy.wait()
    spread.start()
    for copy in into[3:]:
        copy.wait()
    tokens = ((held[3], xn_o), (held[4], xp_o), (held[5], go_o))
    token_copies = [
        remote(a, b.at[t], tsend.at[i, k], trecv.at[i, t], (f, lax.rem(t + k, tp)))
        for i, (a, b) in enumerate(tokens) for k in range(1, tp)
    ]
    slices = held[6]
    slice_copies = []
    for k in range(1, fs):
        other = lax.rem(f + k, fs)
        slice_copies.append(
            remote(slices.at[other], cols_o.at[f, t], csend.at[k], crecv.at[f], (other, t)))
    for copy in token_copies + slice_copies:
        copy.start()
    out = stage_in(
        [(held[0], gate_o.at[f]), (held[1], up_o.at[f]), (held[2], down_o.at[f]),
         (held[3], xn_o.at[t]), (held[4], xp_o.at[t]), (held[5], go_o.at[t]),
         (slices.at[f], cols_o.at[f, t])], lout)
    spread.relay(lambda c: c.start(), True)
    out[6].wait()
    for k in range(1, fs):
        other = lax.rem(f + k, fs)
        mine = cols_o.at[other, t]
        remote(mine, mine, csend.at[k], crecv.at[other], (f, t)).wait_recv()
    mine = cols_o.at[:, t]
    share = [remote(mine, mine, dsend.at[k], drecv.at[t], (f, lax.rem(t + k, tp)))
             for k in range(1, tp)]
    for copy in share:
        copy.start()
    for k in range(1, tp):
        other = lax.rem(t + k, tp)
        for i, (_, b) in enumerate(tokens):
            remote(b.at[other], b.at[other], tsend.at[i, k], trecv.at[i, other], (f, t)).wait_recv()
        theirs = cols_o.at[:, other]
        remote(theirs, theirs, dsend.at[k], drecv.at[other], (f, t)).wait_recv()
    spread.finish()
    for copy in token_copies + slice_copies + share:
        copy.wait_send()
    for copy in out[:6]:
        copy.wait()


def gather_terms(fs, tp, *refs):
    (gg, gu, hp, pn, pp, gg_o, gu_o, hp_o, pn_o, pp_o, *rest) = refs
    held, (wsend, wrecv, tsend, trecv, lin, lout) = rest[:5], rest[5:]
    f, t = lax.axis_index("fs"), lax.axis_index("tp")
    into = stage_in(list(zip((gg, gu, hp, pn, pp), held)), lin)
    spread = Spread(fs, held[:3], (gg_o, gu_o, hp_o), wsend, wrecv)
    for copy in into[:3]:
        copy.wait()
    spread.start()
    for copy in into[3:]:
        copy.wait()
    parts = ((held[3], pn_o), (held[4], pp_o))
    part_copies = []
    for i, (a, b) in enumerate(parts):
        for k in range(1, tp):
            other = lax.rem(t + k, tp)
            part_copies.append(
                remote(a.at[other], b.at[t], tsend.at[i, k], trecv.at[i, t], (f, other)))
    for copy in part_copies:
        copy.start()
    out = stage_in(
        [(held[0], gg_o.at[f]), (held[1], gu_o.at[f]), (held[2], hp_o.at[f]),
         (held[3].at[t], pn_o.at[t]), (held[4].at[t], pp_o.at[t])], lout)
    spread.relay(lambda c: c.start(), True)
    for i, (_, b) in enumerate(parts):
        for k in range(1, tp):
            other = lax.rem(t + k, tp)
            remote(b.at[other], b.at[other], tsend.at[i, k], trecv.at[i, other], (f, t)).wait_recv()
    spread.finish()
    for copy in part_copies:
        copy.wait_send()
    for copy in out:
        copy.wait()


def communicate(body, fs, tp, args, shapes, extra, name):
    n = len(args)
    return pl.pallas_call(
        lambda *refs: body(fs, tp, *refs),
        out_shape=[jax.ShapeDtypeStruct(s, jnp.bfloat16) for s in shapes],
        in_specs=[ANY] * n,
        out_specs=[ANY] * len(shapes),
        scratch_shapes=[pltpu.VMEM(a.shape, a.dtype) for a in args]
        + [pltpu.SemaphoreType.DMA((3, columns_of(fs) + 1, fs)), pltpu.SemaphoreType.DMA((3, fs)),
           pltpu.SemaphoreType.DMA((3, tp)), pltpu.SemaphoreType.DMA((3, tp))]
        + extra
        + [pltpu.SemaphoreType.DMA((n,)), pltpu.SemaphoreType.DMA((n,))],
        compiler_params=pltpu.CompilerParams(has_side_effects=True),
        name=name,
    )(*args)


def local(x_next, x_prev, grad_out, gate_w, up_w, down_w, acc_gate, acc_up, acc_down):
    fs, tp = lax.axis_size("fs"), lax.axis_size("tp")
    rows, model = x_prev.shape
    depth, width = gate_w.shape
    factor = 1.0 / math.sqrt(rows * tp * fs)
    cols = jnp.concatenate(
        (x_prev.reshape(rows, fs, depth), grad_out.reshape(rows, fs, depth)), axis=2
    ).transpose(1, 0, 2)
    sems = pltpu.SemaphoreType.DMA
    gate_full, up_full, down_full, piece, rows_prev, cotangent, all_cols = communicate(
        gather_inputs, fs, tp, (gate_w.T, up_w.T, down_w, x_next, x_prev, grad_out, cols),
        [(fs, width, depth)] * 3
        + [(tp, rows, model)] * 3 + [(fs, tp, rows, 2 * depth)],
        [sems((fs,)), sems((fs,)), sems((tp,)), sems((tp,))], "gather_inputs",
    )
    gate_full, up_full, down_full = (
        a.transpose(1, 0, 2).reshape(width, model) for a in (gate_full, up_full, down_full)
    )
    piece, rows_prev, cotangent = (a.reshape(tp * rows, model) for a in (piece, rows_prev, cotangent))
    x_cols = all_cols[..., :depth].reshape(fs * tp * rows, depth)
    g_cols = all_cols[..., depth:].reshape(fs * tp * rows, depth)

    gate, upper = contract_cols(piece, gate_full), contract_cols(piece, up_full)
    hidden = (jax.nn.silu(gate) * upper).astype(jnp.bfloat16)
    part_next = jnp.dot(hidden, down_full, preferred_element_type=jnp.float32).astype(jnp.bfloat16)
    gate_prev, up_prev = contract_cols(rows_prev, gate_full), contract_cols(rows_prev, up_full)
    grad_hidden = contract_cols(cotangent, down_full)
    sigmoid_gate = jax.nn.sigmoid(gate_prev)
    silu_gate = gate_prev * sigmoid_gate
    grad_gate = (
        grad_hidden * up_prev * sigmoid_gate * (1.0 + gate_prev * (1.0 - sigmoid_gate))
    ).astype(jnp.bfloat16)
    grad_up = (grad_hidden * silu_gate).astype(jnp.bfloat16)
    hidden_prev = (silu_gate * up_prev).astype(jnp.bfloat16)
    part_prev = (
        jnp.dot(grad_gate, gate_full, preferred_element_type=jnp.float32)
        + jnp.dot(grad_up, up_full, preferred_element_type=jnp.float32)
    ).astype(jnp.bfloat16)

    all_gate, all_up, all_hidden, parts_next, parts_prev = communicate(
        gather_terms, fs, tp,
        (grad_gate, grad_up, hidden_prev,
         part_next.reshape(tp, rows, model), part_prev.reshape(tp, rows, model)),
        [(fs, tp * rows, width)] * 3 + [(tp, rows, model)] * 2, [], "gather_terms",
    )
    all_gate, all_up, all_hidden = (a.reshape(fs * tp * rows, width) for a in (all_gate, all_up, all_hidden))
    new_gate = acc_gate + factor * contract_rows(x_cols, all_gate)
    new_up = acc_up + factor * contract_rows(x_cols, all_up)
    new_down = acc_down + factor * contract_rows(all_hidden, g_cols)
    summed = parts_next.astype(jnp.float32).sum(0).astype(jnp.bfloat16)
    grad_input = parts_prev.astype(jnp.float32).sum(0).astype(jnp.bfloat16)
    return (summed, hidden, grad_input, new_gate, new_up, new_down)


def step_kernel(nz, ny, nx, *refs):
    (gate, up, down, xn, xp, go,
     out_o, gin_o, hid_o, terms_o,
     W, X, C, AT, AN, G, U, hn, P, Q, S, T, O, DW, DP,
     wsend, wrecv, ysend, tsend, trecv, csend, crecv, fsend, frecv,
     gsend, grecv, psend, precv, qsend, qrecv, hsend, hrecv, dsend, drecv, osem) = refs
    fs, tp = nz * ny, 2 * nx
    nh, groups, blocks = nz // 2, nz // 2 * ny, 2 * nx
    width, depth = gate.shape
    half = width // 2
    rows, model = xp.shape
    layer = tp * rows
    f, t = lax.axis_index("fs"), lax.axis_index("tp")
    z, y = f // ny, lax.rem(f, ny)
    x, c = t // 2, lax.rem(t, 2)
    h, l = z // 2, lax.rem(z, 2)
    pair = z + 1 - 2 * l
    mine, group = l * tp + t, h * ny + y

    def dev(x, y, z, c):
        return (z * ny + y, x * 2 + c)

    here = dev(x, y, z, c)
    sibling = dev(x, y, z, 1 - c)
    pending = []

    def send(cond, source, target, ssem, rsem, device):
        def start():
            remote(source, target, ssem, rsem, device).start()

        if cond is None:
            start()
        else:
            pl.when(cond)(start)
        pending.append((cond, source, target, ssem, rsem, device))

    def arrived(ref, ssem, rsem):
        remote(ref, ref, ssem, rsem, here).wait_recv()

    def around(size, at):
        return [lax.rem(at + k, size) for k in range(1, size)]

    tokens = (xp, go, xn)

    def block(i):
        return pl.ds(pl.multiple_of(i * rows, 16), rows)

    def token_targets(first):
        out = [(1, sibling)]
        if first:
            out = [(0, dev(x, y, pair, c))] + [
                (1 + k, dev(lax.rem(x + k, nx), y, z, c)) for k in range(1, nx)] + out
        return out

    for m in range(3):
        pltpu.make_async_copy(tokens[m], X.at[m, block(mine)], trecv.at[m, mine]).start()
        for kind, device in token_targets(True):
            send(None, tokens[m], X.at[m, block(mine)], tsend.at[m, mine, kind],
                 trecv.at[m, mine], device)

    mats = (gate, up, down)

    def rows_of(m, cc):
        return mats[m].at[pl.ds(pl.multiple_of(cc * half, 16), half)]

    def own_layer():
        for m in range(3):
            pltpu.make_async_copy(rows_of(m, c), W.at[m, f], wrecv.at[m, f]).start()

    pl.when(c == l)(own_layer)
    for m in range(3):
        send(c == l, rows_of(m, 1 - c), W.at[m, f], wsend.at[m, z, 1 - c], wrecv.at[m, f], sibling)
    for d in range(nz - 1, 0, -1):
        for m in range(3):
            for zc, inside in ((z + d, z + d < nz), (z - d, z - d >= 0)):
                for cc in range(2):
                    send(jnp.logical_and(inside, lax.rem(zc + 2 * nz, 2) == c),
                         rows_of(m, cc), W.at[m, f], wsend.at[m, lax.rem(zc + 2 * nz, nz), cc],
                         wrecv.at[m, f], dev(x, y, zc, cc))

    others = [(dh, dy) for dh in range(nh) for dy in range(ny) if dh or dy]
    for dh, dy in others:
        hh, yy = lax.rem(h + dh, nh), lax.rem(y + dy, ny)
        for m in range(2):
            for ls in range(2):
                at = ((2 * hh + ls) * ny + yy) * depth
                send(None, tokens[m].at[:, pl.ds(pl.multiple_of(at, 128), depth)],
                     C.at[2 * m + ls, group, block(mine)],
                     csend.at[2 * m + ls, hh * ny + yy], crecv.at[2 * m + ls, group],
                     dev(x, yy, 2 * hh + l, c))

    def forward_weight(m, zz):
        s = zz * ny + y
        arrived(W.at[m, s], ysend.at[m, zz, 0], wrecv.at[m, s])
        for k in range(1, ny):
            remote(W.at[m, s], W.at[m, s], ysend.at[m, zz, k], wrecv.at[m, s],
                   dev(x, lax.rem(y + k, ny), z, c)).start()

    def forward_token(i, first):
        for m in range(3):
            arrived(X.at[m, block(i)], tsend.at[m, i, 0], trecv.at[m, i])
            for kind, device in token_targets(True)[1:] if first else token_targets(False):
                send(None, X.at[m, block(i)], X.at[m, block(i)], tsend.at[m, i, kind],
                     trecv.at[m, i], device)

    def forward_column(m, step):
        for d in step:
            pl.when(z + d < nz)(lambda d=d: forward_weight(m, z + d))
            pl.when(z - d >= 0)(lambda d=d: forward_weight(m, z - d))

    for m in range(3):
        forward_weight(m, z)
    forward_token((1 - l) * tp + t, True)
    for xx in around(nx, x):
        forward_token(l * tp + xx * 2 + c, False)
    forward_column(0, range(1, nz))
    for xx in around(nx, x):
        forward_token((1 - l) * tp + xx * 2 + c, False)
    forward_column(1, range(1, nz))
    forward_column(2, range(1, nz))

    for m in range(3):
        arrived(X.at[m, block(mine)], tsend.at[m, mine, 0], trecv.at[m, mine])
        for ll in range(2):
            for xx in range(nx):
                i = ll * tp + xx * 2 + 1 - c
                arrived(X.at[m, block(i)], tsend.at[m, i, 0], trecv.at[m, i])

    AT[...] = jnp.zeros_like(AT)
    AN[...] = jnp.zeros_like(AN)

    def slice_products(s):
        at = pl.ds(pl.multiple_of(s * depth, 128), depth)
        p, g, n = X[0, :, at], X[1, :, at], X[2, :, at]
        AT[0] += contract_cols(W[0, s], p)
        AT[1] += contract_cols(W[1, s], p)
        AT[2] += contract_cols(W[2, s], g)
        AN[0] += contract_cols(n, W[0, s])
        AN[1] += contract_cols(n, W[1, s])

    def own_column(k, carry):
        slice_products(k * ny + y)
        return carry

    lax.fori_loop(0, nz, own_column, 0)

    def other_column(yy, k, carry):
        s = lax.rem(z + k, nz) * ny + yy
        for m in range(3):
            arrived(W.at[m, s], ysend.at[m, 0, 0], wrecv.at[m, s])
        slice_products(s)
        return carry

    for yy in around(ny, y):
        lax.fori_loop(0, nz, lambda k, carry, yy=yy: other_column(yy, k, carry), 0)

    part = math.gcd(half, 32)

    def gradients(r, carry):
        at = pl.ds(pl.multiple_of(r * part, part), part)
        g, u, gh = AT[0, at], AT[1, at], AT[2, at]
        s = jax.nn.sigmoid(g)
        sg = g * s
        G[0, group, at] = (gh * u * s * (1.0 + g * (1.0 - s))).astype(jnp.bfloat16)
        G[1, group, at] = (gh * sg).astype(jnp.bfloat16)
        G[2, group, at] = (sg * u).astype(jnp.bfloat16)
        return carry

    lax.fori_loop(0, half // part, gradients, 0)
    step = math.gcd(rows, 32)

    def activations(r, carry):
        at = pl.ds(pl.multiple_of(r * step, step), step)
        g = AN[0, at]
        hn[at] = (g * jax.nn.sigmoid(g) * AN[1, at]).astype(jnp.bfloat16)
        return carry

    lax.fori_loop(0, 2 * layer // step, activations, 0)

    for m in range(3):
        for k in range(1, nh):
            hh = lax.rem(h + k, nh)
            send(None, G.at[m, group], G.at[m, group], gsend.at[m, group, k - 1],
                 grecv.at[m, group], dev(x, y, 2 * hh + l, c))
        for k in range(1, ny):
            send(None, G.at[m, group], G.at[m, group], gsend.at[m, group, nh + k - 1],
                 grecv.at[m, group], dev(x, lax.rem(y + k, ny), z, c))

    for ll in range(2):
        source = hn.at[pl.ds(ll * layer, layer)]
        alone = jnp.logical_and(l == ll, c == l)
        pl.when(alone)(lambda source=source: pltpu.make_async_copy(
            source, hid_o.at[c], hrecv.at[c]).start())
        send(jnp.logical_not(alone), source, hid_o.at[c], hsend.at[ll], hrecv.at[c],
             dev(x, y, 2 * h + ll, l))

    def column_targets(first):
        return [(kind, device) for kind, device in token_targets(first)]

    def forward_columns(i, targets, direct):
        for dh, dy in others:
            g = lax.rem(h + dh, nh) * ny + lax.rem(y + dy, ny)
            if direct:
                for j in range(4):
                    arrived(C.at[j, g, block(i)], csend.at[j, g], crecv.at[j, g])
            else:
                arrived(C.at[:, g, block(i)], fsend.at[g, i, 0], frecv.at[g, i])
            for kind, device in targets:
                send(None, C.at[:, g, block(i)], C.at[:, g, block(i)], fsend.at[g, i, kind],
                     frecv.at[g, i], device)

    forward_columns(mine, token_targets(True), True)

    U[0] = G[0, group].T
    U[1] = G[1, group].T

    def shares(s, carry):
        at = pl.ds(pl.multiple_of(s * depth, 128), depth)
        P[0, :, at] = jnp.dot(
            hn[...], W[2, s], preferred_element_type=jnp.float32).astype(jnp.bfloat16)
        P[1, :, at] = (
            jnp.dot(U[0], W[0, s], preferred_element_type=jnp.float32)
            + jnp.dot(U[1], W[1, s], preferred_element_type=jnp.float32)
        ).astype(jnp.bfloat16)
        return carry

    lax.fori_loop(0, fs, shares, 0)

    forward_columns((1 - l) * tp + t, token_targets(True)[1:], False)
    for ll in range(2):
        for xx in range(nx):
            i = ll * tp + xx * 2 + 1 - c
            for p in range(2):
                send(None, P.at[p, block(i)], Q.at[p, ll * nx + xx], psend.at[p, ll * nx + xx],
                     precv.at[p, ll * nx + xx], sibling)

    for m in range(2):
        for ls in range(2):
            at = ((2 * h + ls) * ny + y) * depth
            C[2 * m + ls, group] = X[m, :, pl.ds(pl.multiple_of(at, 128), depth)]

    def weight_terms(m, g, first):
        for ls in range(2):
            value = jnp.dot(G[m, g], C[(2 if m == 2 else 0) + ls, g],
                            preferred_element_type=jnp.float32)
            if first:
                DW[ls, m] = value
            else:
                DW[ls, m] += value

    for m in range(3):
        weight_terms(m, group, True)

    spot = l * nx + x
    for ll in range(2):
        for xx in range(nx):
            b = ll * nx + xx
            i = ll * tp + xx * 2 + c
            for p in range(2):
                arrived(Q.at[p, b], psend.at[p, b], precv.at[p, b])
                S[p, b] = (P[p, block(i)].astype(jnp.float32)
                           + Q[p, b].astype(jnp.float32)).astype(jnp.bfloat16)
    for ll in range(2):
        for xx in range(nx):
            b = ll * nx + xx
            for p in range(2):
                send(b != spot, S.at[p, b], T.at[p, spot], qsend.at[p, b], qrecv.at[p, spot],
                     dev(xx, y, 2 * h + ll, c))

    for xx in around(nx, x):
        forward_columns(l * tp + xx * 2 + c, token_targets(False), False)
        forward_columns((1 - l) * tp + xx * 2 + c, token_targets(False), False)
    for ll in range(2):
        for xx in range(nx):
            i = ll * tp + xx * 2 + 1 - c
            for dh, dy in others:
                g = lax.rem(h + dh, nh) * ny + lax.rem(y + dy, ny)
                arrived(C.at[:, g, block(i)], fsend.at[g, i, 0], frecv.at[g, i])

    def relay_terms(m):
        for k in range(1, nh):
            g = lax.rem(h + k, nh) * ny + y
            arrived(G.at[m, g], gsend.at[m, g, 0], grecv.at[m, g])
            for j in range(1, ny):
                send(None, G.at[m, g], G.at[m, g], gsend.at[m, g, nh + j - 1], grecv.at[m, g],
                     dev(x, lax.rem(y + j, ny), z, c))

    relay_terms(0)
    for m in range(3):
        for k in range(1, nh):
            weight_terms(m, lax.rem(h + k, nh) * ny + y, False)
        for j in range(1, ny):
            g = h * ny + lax.rem(y + j, ny)
            arrived(G.at[m, g], gsend.at[m, g, 0], grecv.at[m, g])
            weight_terms(m, g, False)
        if m + 1 < 3:
            relay_terms(m + 1)
        for k in range(1, nh):
            for j in range(1, ny):
                g = lax.rem(h + k, nh) * ny + lax.rem(y + j, ny)
                arrived(G.at[m, g], gsend.at[m, g, 0], grecv.at[m, g])
                weight_terms(m, g, False)
        DP[0, m] = DW[1 - l, m].astype(jnp.bfloat16)
        DP[1, m] = DW[l, m].astype(jnp.bfloat16)
        send(None, DP.at[0, m], terms_o.at[c, m], dsend.at[0, m], drecv.at[c, m],
             dev(x, y, pair, l))
        pl.when(c == l)(lambda m=m: pltpu.make_async_copy(
            DP.at[1, m], terms_o.at[c, m], drecv.at[c, m]).start())
        send(c != l, DP.at[1, m], terms_o.at[c, m], dsend.at[1, m], drecv.at[c, m], sibling)

    for p in range(2):
        total = S[p, spot].astype(jnp.float32)
        for b in range(blocks):
            pl.when(b != spot)(lambda p=p, b=b: arrived(
                T.at[p, b], qsend.at[p, b], qrecv.at[p, b]))
        for k in range(1, blocks):
            total += T[p, lax.rem(spot + k, blocks)].astype(jnp.float32)
        O[p] = total.astype(jnp.bfloat16)
    results = [pltpu.make_async_copy(O.at[p], ref, osem.at[p])
               for p, ref in enumerate((out_o, gin_o))]

    for cond, *copy in pending:
        def finish(copy=copy):
            remote(*copy).wait_send()

        if cond is None:
            finish()
        else:
            pl.when(cond)(finish)
    for copy in results:
        copy.start()
    for m in range(3):
        for zz in range(nz):
            s = zz * ny + y
            for k in range(1, ny):
                remote(W.at[m, s], W.at[m, s], ysend.at[m, zz, k], wrecv.at[m, s],
                       dev(x, lax.rem(y + k, ny), z, c)).wait_send()
    for cc in range(2):
        arrived(hid_o.at[cc], hsend.at[cc], hrecv.at[cc])
        for m in range(3):
            arrived(terms_o.at[cc, m], dsend.at[0, m], drecv.at[cc, m])
    for copy in results:
        copy.wait()


def layered(x_next, x_prev, grad_out, gate_w, up_w, down_w, acc_gate, acc_up, acc_down):
    fs, tp = lax.axis_size("fs"), lax.axis_size("tp")
    ny = columns_of(fs)
    nz, nx = fs // ny, tp // 2
    rows, model = x_prev.shape
    depth, width = gate_w.shape
    half, tokens = width // 2, 2 * tp * rows
    groups, blocks = nz // 2 * ny, 2 * nx
    factor = 1.0 / math.sqrt(rows * tp * fs)
    bf, sems = jnp.bfloat16, pltpu.SemaphoreType.DMA
    out_next, grad_input, hidden, terms = pl.pallas_call(
        lambda *refs: step_kernel(nz, ny, nx, *refs),
        out_shape=[jax.ShapeDtypeStruct(s, bf) for s in (
            (rows, model), (rows, model), (2, tp * rows, half), (2, 3, half, depth))],
        in_specs=[ANY] * 6,
        out_specs=[ANY] * 4,
        scratch_shapes=[
            pltpu.VMEM((3, fs, half, depth), bf),
            pltpu.VMEM((3, tokens, model), bf),
            pltpu.VMEM((4, groups, tokens, depth), bf),
            pltpu.VMEM((3, half, tokens), jnp.float32),
            pltpu.VMEM((2, tokens, half), jnp.float32),
            pltpu.VMEM((3, groups, half, tokens), bf),
            pltpu.VMEM((2, tokens, half), bf),
            pltpu.VMEM((tokens, half), bf),
            pltpu.VMEM((2, tokens, model), bf),
            pltpu.VMEM((2, blocks, rows, model), bf),
            pltpu.VMEM((2, blocks, rows, model), bf),
            pltpu.VMEM((2, blocks, rows, model), bf),
            pltpu.VMEM((2, rows, model), bf),
            pltpu.VMEM((2, 3, half, depth), jnp.float32),
            pltpu.VMEM((2, 3, half, depth), bf),
            sems((3, nz, 2)), sems((3, fs)), sems((3, nz, ny)),
            sems((3, 2 * tp, nx + 1)), sems((3, 2 * tp)),
            sems((4, groups)), sems((4, groups)),
            sems((groups, 2 * tp, nx + 1)), sems((groups, 2 * tp)),
            sems((3, groups, nz // 2 + ny)), sems((3, groups)),
            sems((2, blocks)), sems((2, blocks)), sems((2, blocks)), sems((2, blocks)),
            sems((2,)), sems((2,)), sems((2, 3)), sems((2, 3)), sems((2,)),
        ],
        compiler_params=pltpu.CompilerParams(has_side_effects=True),
        name="step",
    )(gate_w.T, up_w.T, down_w, x_next, x_prev, grad_out)
    saved = jnp.concatenate((hidden[0], hidden[1]), axis=1)

    def updated(acc, m):
        return acc + factor * terms[:, m].reshape(width, depth).astype(jnp.float32)

    return (out_next, saved, grad_input,
            updated(acc_gate.T, 0).T, updated(acc_up.T, 1).T, updated(acc_down, 2))


def layers_fit(fs, tp, rows, depth, width):
    nz = fs // columns_of(fs)
    return nz % 2 == 0 and tp % 2 == 0 and depth % 128 == 0 and width % 32 == 0 and rows % 16 == 0


def choose(*args):
    depth, width = args[3].shape
    fits = layers_fit(lax.axis_size("fs"), lax.axis_size("tp"), args[0].shape[0], depth, width)
    return (layered if fits else local)(*args)


def solution(mesh):
    in_specs = (
        P(("fs", "tp"), None),
        P(("fs", "tp"), None),
        P(("fs", "tp"), None),
        P("fs", "tp"),
        P("fs", "tp"),
        P("tp", "fs"),
        P("fs", "tp"),
        P("fs", "tp"),
        P("tp", "fs"),
    )
    out_specs = (
        P(("fs", "tp"), None),
        P("fs", "tp"),
        P(("fs", "tp"), None),
        P("fs", "tp"),
        P("fs", "tp"),
        P("tp", "fs"),
    )
    return jax.shard_map(choose, mesh=mesh, in_specs=in_specs, out_specs=out_specs, check_vma=False)
```

```python
import math

import jax
import jax.numpy as jnp
from jax import lax
from jax.experimental import pallas as pl
from jax.experimental.pallas import tpu as pltpu
from jax.sharding import PartitionSpec as P

MESH = pl.DeviceIdType.MESH
ANY = pl.BlockSpec(memory_space=pl.ANY)


def columns_of(size):
    side = 1
    while 8 * side * side <= size and size % (2 * side) == 0:
        side *= 2
    return side


def contract_rows(left, right):
    return lax.dot_general(
        left, right, (((0,), (0,)), ((), ())), preferred_element_type=jnp.float32
    )


def contract_cols(left, right):
    return lax.dot_general(
        left, right, (((1,), (1,)), ((), ())), preferred_element_type=jnp.float32
    )


def remote(source, target, send, recv, device):
    return pltpu.make_async_remote_copy(
        src_ref=source, dst_ref=target, send_sem=send, recv_sem=recv,
        device_id=device, device_id_type=MESH,
    )


class Spread:
    def __init__(self, fs, owns, fulls, send, recv):
        self.ny = columns_of(fs)
        self.nz = fs // self.ny
        self.fs, self.owns, self.fulls = fs, owns, fulls
        self.send, self.recv = send, recv
        self.f, self.t = lax.axis_index("fs"), lax.axis_index("tp")
        self.z, self.y = self.f // self.ny, lax.rem(self.f, self.ny)

    def flows(self, w, f, source, up, down, act):
        full = self.fulls[w].at[f]

        def go(kind, z, y):
            act(remote(source, full, self.send.at[w, kind, f], self.recv.at[w, f],
                       (z * self.ny + y, self.t)))

        if up:
            pl.when(self.z + 1 < self.nz)(lambda: go(0, self.z + 1, self.y))
        if down:
            pl.when(self.z > 0)(lambda: go(1, self.z - 1, self.y))
        for k in range(1, self.ny):
            go(1 + k, self.z, lax.rem(self.y + k, self.ny))

    def start(self):
        for w, own in enumerate(self.owns):
            self.flows(w, self.f, own, True, True, lambda c: c.start())

    def arrived(self, w, f):
        full = self.fulls[w].at[f]
        remote(full, full, self.send.at[w, 0, f], self.recv.at[w, f],
               (self.f, self.t)).wait_recv()

    def relay(self, act, wait):
        for d in range(1, self.nz):
            for w in range(len(self.owns)):
                def from_below(w=w, d=d):
                    f = (self.z - d) * self.ny + self.y
                    if wait:
                        self.arrived(w, f)
                    self.flows(w, f, self.fulls[w].at[f], True, False, act)

                def from_above(w=w, d=d):
                    f = (self.z + d) * self.ny + self.y
                    if wait:
                        self.arrived(w, f)
                    self.flows(w, f, self.fulls[w].at[f], False, True, act)

                pl.when(self.z >= d)(from_below)
                pl.when(self.z + d < self.nz)(from_above)

    def finish(self):
        for w in range(len(self.owns)):
            for z in range(self.nz):
                for k in range(1, self.ny):
                    self.arrived(w, z * self.ny + lax.rem(self.y + k, self.ny))
        for w, own in enumerate(self.owns):
            self.flows(w, self.f, own, True, True, lambda c: c.wait_send())
        self.relay(lambda c: c.wait_send(), False)


def stage_in(pairs, sem):
    copies = [pltpu.make_async_copy(a, b, sem.at[i]) for i, (a, b) in enumerate(pairs)]
    for copy in copies:
        copy.start()
    return copies


def gather_inputs(fs, tp, *refs):
    (gate, up, down, xn, xp, go, cols,
     gate_o, up_o, down_o, xn_o, xp_o, go_o, cols_o,
     *rest) = refs
    held, (wsend, wrecv, tsend, trecv, csend, crecv, dsend, drecv, lin, lout) = rest[:7], rest[7:]
    f, t = lax.axis_index("fs"), lax.axis_index("tp")
    sources = (gate, up, down, xn, xp, go, cols)
    into = stage_in(list(zip(sources, held)), lin)
    spread = Spread(fs, held[:3], (gate_o, up_o, down_o), wsend, wrecv)
    for copy in into[:3]:
        copy.wait()
    spread.start()
    for copy in into[3:]:
        copy.wait()
    tokens = ((held[3], xn_o), (held[4], xp_o), (held[5], go_o))
    token_copies = [
        remote(a, b.at[t], tsend.at[i, k], trecv.at[i, t], (f, lax.rem(t + k, tp)))
        for i, (a, b) in enumerate(tokens) for k in range(1, tp)
    ]
    slices = held[6]
    slice_copies = []
    for k in range(1, fs):
        other = lax.rem(f + k, fs)
        slice_copies.append(
            remote(slices.at[other], cols_o.at[f, t], csend.at[k], crecv.at[f], (other, t)))
    for copy in token_copies + slice_copies:
        copy.start()
    out = stage_in(
        [(held[0], gate_o.at[f]), (held[1], up_o.at[f]), (held[2], down_o.at[f]),
         (held[3], xn_o.at[t]), (held[4], xp_o.at[t]), (held[5], go_o.at[t]),
         (slices.at[f], cols_o.at[f, t])], lout)
    spread.relay(lambda c: c.start(), True)
    out[6].wait()
    for k in range(1, fs):
        other = lax.rem(f + k, fs)
        mine = cols_o.at[other, t]
        remote(mine, mine, csend.at[k], crecv.at[other], (f, t)).wait_recv()
    mine = cols_o.at[:, t]
    share = [remote(mine, mine, dsend.at[k], drecv.at[t], (f, lax.rem(t + k, tp)))
             for k in range(1, tp)]
    for copy in share:
        copy.start()
    for k in range(1, tp):
        other = lax.rem(t + k, tp)
        for i, (_, b) in enumerate(tokens):
            remote(b.at[other], b.at[other], tsend.at[i, k], trecv.at[i, other], (f, t)).wait_recv()
        theirs = cols_o.at[:, other]
        remote(theirs, theirs, dsend.at[k], drecv.at[other], (f, t)).wait_recv()
    spread.finish()
    for copy in token_copies + slice_copies + share:
        copy.wait_send()
    for copy in out[:6]:
        copy.wait()


def gather_terms(fs, tp, *refs):
    (gg, gu, hp, pn, pp, gg_o, gu_o, hp_o, pn_o, pp_o, *rest) = refs
    held, (wsend, wrecv, tsend, trecv, lin, lout) = rest[:5], rest[5:]
    f, t = lax.axis_index("fs"), lax.axis_index("tp")
    into = stage_in(list(zip((gg, gu, hp, pn, pp), held)), lin)
    spread = Spread(fs, held[:3], (gg_o, gu_o, hp_o), wsend, wrecv)
    for copy in into[:3]:
        copy.wait()
    spread.start()
    for copy in into[3:]:
        copy.wait()
    parts = ((held[3], pn_o), (held[4], pp_o))
    part_copies = []
    for i, (a, b) in enumerate(parts):
        for k in range(1, tp):
            other = lax.rem(t + k, tp)
            part_copies.append(
                remote(a.at[other], b.at[t], tsend.at[i, k], trecv.at[i, t], (f, other)))
    for copy in part_copies:
        copy.start()
    out = stage_in(
        [(held[0], gg_o.at[f]), (held[1], gu_o.at[f]), (held[2], hp_o.at[f]),
         (held[3].at[t], pn_o.at[t]), (held[4].at[t], pp_o.at[t])], lout)
    spread.relay(lambda c: c.start(), True)
    for i, (_, b) in enumerate(parts):
        for k in range(1, tp):
            other = lax.rem(t + k, tp)
            remote(b.at[other], b.at[other], tsend.at[i, k], trecv.at[i, other], (f, t)).wait_recv()
    spread.finish()
    for copy in part_copies:
        copy.wait_send()
    for copy in out:
        copy.wait()


def communicate(body, fs, tp, args, shapes, extra, name):
    n = len(args)
    return pl.pallas_call(
        lambda *refs: body(fs, tp, *refs),
        out_shape=[jax.ShapeDtypeStruct(s, jnp.bfloat16) for s in shapes],
        in_specs=[ANY] * n,
        out_specs=[ANY] * len(shapes),
        scratch_shapes=[pltpu.VMEM(a.shape, a.dtype) for a in args]
        + [pltpu.SemaphoreType.DMA((3, columns_of(fs) + 1, fs)), pltpu.SemaphoreType.DMA((3, fs)),
           pltpu.SemaphoreType.DMA((3, tp)), pltpu.SemaphoreType.DMA((3, tp))]
        + extra
        + [pltpu.SemaphoreType.DMA((n,)), pltpu.SemaphoreType.DMA((n,))],
        compiler_params=pltpu.CompilerParams(has_side_effects=True),
        name=name,
    )(*args)


def local(x_next, x_prev, grad_out, gate_w, up_w, down_w, acc_gate, acc_up, acc_down):
    fs, tp = lax.axis_size("fs"), lax.axis_size("tp")
    rows, model = x_prev.shape
    depth, width = gate_w.shape
    factor = 1.0 / math.sqrt(rows * tp * fs)
    cols = jnp.concatenate(
        (x_prev.reshape(rows, fs, depth), grad_out.reshape(rows, fs, depth)), axis=2
    ).transpose(1, 0, 2)
    sems = pltpu.SemaphoreType.DMA
    gate_full, up_full, down_full, piece, rows_prev, cotangent, all_cols = communicate(
        gather_inputs, fs, tp, (gate_w.T, up_w.T, down_w, x_next, x_prev, grad_out, cols),
        [(fs, width, depth)] * 3
        + [(tp, rows, model)] * 3 + [(fs, tp, rows, 2 * depth)],
        [sems((fs,)), sems((fs,)), sems((tp,)), sems((tp,))], "gather_inputs",
    )
    gate_full, up_full, down_full = (
        a.transpose(1, 0, 2).reshape(width, model) for a in (gate_full, up_full, down_full)
    )
    piece, rows_prev, cotangent = (a.reshape(tp * rows, model) for a in (piece, rows_prev, cotangent))
    x_cols = all_cols[..., :depth].reshape(fs * tp * rows, depth)
    g_cols = all_cols[..., depth:].reshape(fs * tp * rows, depth)

    gate, upper = contract_cols(piece, gate_full), contract_cols(piece, up_full)
    hidden = (jax.nn.silu(gate) * upper).astype(jnp.bfloat16)
    part_next = jnp.dot(hidden, down_full, preferred_element_type=jnp.float32).astype(jnp.bfloat16)
    gate_prev, up_prev = contract_cols(rows_prev, gate_full), contract_cols(rows_prev, up_full)
    grad_hidden = contract_cols(cotangent, down_full)
    sigmoid_gate = jax.nn.sigmoid(gate_prev)
    silu_gate = gate_prev * sigmoid_gate
    grad_gate = (
        grad_hidden * up_prev * sigmoid_gate * (1.0 + gate_prev * (1.0 - sigmoid_gate))
    ).astype(jnp.bfloat16)
    grad_up = (grad_hidden * silu_gate).astype(jnp.bfloat16)
    hidden_prev = (silu_gate * up_prev).astype(jnp.bfloat16)
    part_prev = (
        jnp.dot(grad_gate, gate_full, preferred_element_type=jnp.float32)
        + jnp.dot(grad_up, up_full, preferred_element_type=jnp.float32)
    ).astype(jnp.bfloat16)

    all_gate, all_up, all_hidden, parts_next, parts_prev = communicate(
        gather_terms, fs, tp,
        (grad_gate, grad_up, hidden_prev,
         part_next.reshape(tp, rows, model), part_prev.reshape(tp, rows, model)),
        [(fs, tp * rows, width)] * 3 + [(tp, rows, model)] * 2, [], "gather_terms",
    )
    all_gate, all_up, all_hidden = (a.reshape(fs * tp * rows, width) for a in (all_gate, all_up, all_hidden))
    new_gate = acc_gate + factor * contract_rows(x_cols, all_gate)
    new_up = acc_up + factor * contract_rows(x_cols, all_up)
    new_down = acc_down + factor * contract_rows(all_hidden, g_cols)
    summed = parts_next.astype(jnp.float32).sum(0).astype(jnp.bfloat16)
    grad_input = parts_prev.astype(jnp.float32).sum(0).astype(jnp.bfloat16)
    return (summed, hidden, grad_input, new_gate, new_up, new_down)


def step_kernel(nz, ny, nx, *refs):
    (gate, up, down, xn, xp, go,
     out_o, gin_o, hid_o, terms_o,
     W, X, C, AT, AN, G, U, hn, P, Q, S, T, O, DW, DP,
     wsend, wrecv, ysend, tsend, trecv, csend, crecv, fsend, frecv,
     gsend, grecv, psend, precv, qsend, qrecv, hsend, hrecv, dsend, drecv, osem) = refs
    fs, tp = nz * ny, 2 * nx
    nh, groups, blocks = nz // 2, nz // 2 * ny, 2 * nx
    width, depth = gate.shape
    half = width // 2
    rows, model = xp.shape
    layer = tp * rows
    f, t = lax.axis_index("fs"), lax.axis_index("tp")
    z, y = f // ny, lax.rem(f, ny)
    x, c = t // 2, lax.rem(t, 2)
    h, l = z // 2, lax.rem(z, 2)
    pair = z + 1 - 2 * l
    mine, group = l * tp + t, h * ny + y

    def dev(x, y, z, c):
        return (z * ny + y, x * 2 + c)

    here = dev(x, y, z, c)
    sibling = dev(x, y, z, 1 - c)
    pending = []

    def send(cond, source, target, ssem, rsem, device):
        def start():
            remote(source, target, ssem, rsem, device).start()

        if cond is None:
            start()
        else:
            pl.when(cond)(start)
        pending.append((cond, source, target, ssem, rsem, device))

    def arrived(ref, ssem, rsem):
        remote(ref, ref, ssem, rsem, here).wait_recv()

    def around(size, at):
        return [lax.rem(at + k, size) for k in range(1, size)]

    barrier = pltpu.get_barrier_semaphore()
    peers = [dev(x, y, lax.rem(z + d, nz), cc) for d in range(1, nz) for cc in range(2)]
    peers += [sibling] + [dev(xx, y, z, c) for xx in around(nx, x)]
    peers += [dev(x, yy, lax.rem(z + 2 * d, nz), c) for yy in around(ny, y) for d in range(nh)]
    for peer in peers:
        pl.semaphore_signal(barrier, inc=1, device_id=peer, device_id_type=MESH)
    pl.semaphore_wait(barrier, len(peers))

    tokens = (xp, go, xn)

    def block(i):
        return pl.ds(pl.multiple_of(i * rows, 16), rows)

    def token_targets(first):
        out = [(1, sibling)]
        if first:
            out = [(0, dev(x, y, pair, c))] + [
                (1 + k, dev(lax.rem(x + k, nx), y, z, c)) for k in range(1, nx)] + out
        return out

    for m in range(3):
        pltpu.make_async_copy(tokens[m], X.at[m, block(mine)], trecv.at[m, mine]).start()
        for kind, device in token_targets(True):
            send(None, tokens[m], X.at[m, block(mine)], tsend.at[m, mine, kind],
                 trecv.at[m, mine], device)

    mats = (gate, up, down)
    piece = half // 2

    def rows_of(q, cc):
        return mats[q // 2].at[pl.ds(pl.multiple_of(cc * half + q % 2 * piece, 16), piece)]

    def slot(q, s):
        return W.at[q // 2, s, pl.ds(q % 2 * piece, piece)]

    def own_layer():
        for q in range(6):
            pltpu.make_async_copy(rows_of(q, c), slot(q, f), wrecv.at[q, f]).start()

    pl.when(c == l)(own_layer)
    for q in range(6):
        send(c == l, rows_of(q, 1 - c), slot(q, f), wsend.at[q, z, 1 - c], wrecv.at[q, f], sibling)
    for q in range(6):
        for d in range(nz - 1, 0, -1):
            for zc, inside in ((z + d, z + d < nz), (z - d, z - d >= 0)):
                for cc in range(2):
                    send(jnp.logical_and(inside, lax.rem(zc + 2 * nz, 2) == c),
                         rows_of(q, cc), slot(q, f), wsend.at[q, lax.rem(zc + 2 * nz, nz), cc],
                         wrecv.at[q, f], dev(x, y, zc, cc))

    others = [(dh, dy) for dh in range(nh) for dy in range(ny) if dh or dy]
    for dh, dy in others:
        hh, yy = lax.rem(h + dh, nh), lax.rem(y + dy, ny)
        for m in range(2):
            for ls in range(2):
                at = ((2 * hh + ls) * ny + yy) * depth
                send(None, tokens[m].at[:, pl.ds(pl.multiple_of(at, 128), depth)],
                     C.at[2 * m + ls, group, block(mine)],
                     csend.at[2 * m + ls, hh * ny + yy], crecv.at[2 * m + ls, group],
                     dev(x, yy, 2 * hh + l, c))

    def forward_weight(q, zz):
        s = zz * ny + y
        arrived(slot(q, s), ysend.at[q, zz, 0], wrecv.at[q, s])
        for k in range(1, ny):
            remote(slot(q, s), slot(q, s), ysend.at[q, zz, k], wrecv.at[q, s],
                   dev(x, lax.rem(y + k, ny), z, c)).start()

    def forward_token(i, first):
        for m in range(3):
            arrived(X.at[m, block(i)], tsend.at[m, i, 0], trecv.at[m, i])
            for kind, device in token_targets(True)[1:] if first else token_targets(False):
                send(None, X.at[m, block(i)], X.at[m, block(i)], tsend.at[m, i, kind],
                     trecv.at[m, i], device)

    def forward_column(m):
        for q in (2 * m, 2 * m + 1):
            for d in range(1, nz):
                pl.when(z + d < nz)(lambda q=q, d=d: forward_weight(q, z + d))
                pl.when(z - d >= 0)(lambda q=q, d=d: forward_weight(q, z - d))

    for q in range(6):
        forward_weight(q, z)
    forward_column(0)
    forward_token((1 - l) * tp + t, True)
    for xx in around(nx, x):
        forward_token(l * tp + xx * 2 + c, False)
    forward_column(1)
    for xx in around(nx, x):
        forward_token((1 - l) * tp + xx * 2 + c, False)
    forward_column(2)
    for m in range(3):
        arrived(X.at[m, block(mine)], tsend.at[m, mine, 0], trecv.at[m, mine])
        for ll in range(2):
            for xx in range(nx):
                i = ll * tp + xx * 2 + 1 - c
                arrived(X.at[m, block(i)], tsend.at[m, i, 0], trecv.at[m, i])

    AT[...] = jnp.zeros_like(AT)
    AN[...] = jnp.zeros_like(AN)

    def slice_products(s):
        at = pl.ds(pl.multiple_of(s * depth, 128), depth)
        p, g, n = X[0, :, at], X[1, :, at], X[2, :, at]
        AT[0] += contract_cols(W[0, s], p)
        AT[1] += contract_cols(W[1, s], p)
        AT[2] += contract_cols(W[2, s], g)
        AN[0] += contract_cols(n, W[0, s])
        AN[1] += contract_cols(n, W[1, s])

    def own_column(k, carry):
        slice_products(k * ny + y)
        return carry

    lax.fori_loop(0, nz, own_column, 0)

    def other_column(yy, k, carry):
        s = lax.rem(z + k, nz) * ny + yy
        for q in range(6):
            arrived(slot(q, s), ysend.at[q, 0, 0], wrecv.at[q, s])
        slice_products(s)
        return carry

    for yy in around(ny, y):
        lax.fori_loop(0, nz, lambda k, carry, yy=yy: other_column(yy, k, carry), 0)

    part = math.gcd(half, 32)

    def gradients(r, carry):
        at = pl.ds(pl.multiple_of(r * part, part), part)
        g, u, gh = AT[0, at], AT[1, at], AT[2, at]
        s = jax.nn.sigmoid(g)
        sg = g * s
        G[0, group, at] = (gh * u * s * (1.0 + g * (1.0 - s))).astype(jnp.bfloat16)
        G[1, group, at] = (gh * sg).astype(jnp.bfloat16)
        G[2, group, at] = (sg * u).astype(jnp.bfloat16)
        return carry

    lax.fori_loop(0, half // part, gradients, 0)
    step = math.gcd(rows, 32)

    def activations(r, carry):
        at = pl.ds(pl.multiple_of(r * step, step), step)
        g = AN[0, at]
        hn[at] = (g * jax.nn.sigmoid(g) * AN[1, at]).astype(jnp.bfloat16)
        return carry

    lax.fori_loop(0, 2 * layer // step, activations, 0)

    for m in range(3):
        for k in range(1, nh):
            hh = lax.rem(h + k, nh)
            send(None, G.at[m, group], G.at[m, group], gsend.at[m, group, k - 1],
                 grecv.at[m, group], dev(x, y, 2 * hh + l, c))
        for k in range(1, ny):
            send(None, G.at[m, group], G.at[m, group], gsend.at[m, group, nh + k - 1],
                 grecv.at[m, group], dev(x, lax.rem(y + k, ny), z, c))

    for ll in range(2):
        source = hn.at[pl.ds(ll * layer, layer)]
        alone = jnp.logical_and(l == ll, c == l)
        pl.when(alone)(lambda source=source: pltpu.make_async_copy(
            source, hid_o.at[c], hrecv.at[c]).start())
        send(jnp.logical_not(alone), source, hid_o.at[c], hsend.at[ll], hrecv.at[c],
             dev(x, y, 2 * h + ll, l))

    def column_targets(first):
        return [(kind, device) for kind, device in token_targets(first)]

    def forward_columns(i, targets, direct):
        for dh, dy in others:
            g = lax.rem(h + dh, nh) * ny + lax.rem(y + dy, ny)
            if direct:
                for j in range(4):
                    arrived(C.at[j, g, block(i)], csend.at[j, g], crecv.at[j, g])
            else:
                arrived(C.at[:, g, block(i)], fsend.at[g, i, 0], frecv.at[g, i])
            for kind, device in targets:
                send(None, C.at[:, g, block(i)], C.at[:, g, block(i)], fsend.at[g, i, kind],
                     frecv.at[g, i], device)

    forward_columns(mine, token_targets(True), True)

    U[0] = G[0, group].T
    U[1] = G[1, group].T

    def shares(s, carry):
        at = pl.ds(pl.multiple_of(s * depth, 128), depth)
        P[0, :, at] = jnp.dot(
            hn[...], W[2, s], preferred_element_type=jnp.float32).astype(jnp.bfloat16)
        P[1, :, at] = (
            jnp.dot(U[0], W[0, s], preferred_element_type=jnp.float32)
            + jnp.dot(U[1], W[1, s], preferred_element_type=jnp.float32)
        ).astype(jnp.bfloat16)
        return carry

    lax.fori_loop(0, fs, shares, 0)
    for ll in range(2):
        for xx in range(nx):
            i = ll * tp + xx * 2 + 1 - c
            for p in range(2):
                send(None, P.at[p, block(i)], Q.at[p, ll * nx + xx], psend.at[p, ll * nx + xx],
                     precv.at[p, ll * nx + xx], sibling)

    for m in range(2):
        for ls in range(2):
            at = ((2 * h + ls) * ny + y) * depth
            C[2 * m + ls, group] = X[m, :, pl.ds(pl.multiple_of(at, 128), depth)]

    def weight_terms(m, g, first):
        for ls in range(2):
            value = jnp.dot(G[m, g], C[(2 if m == 2 else 0) + ls, g],
                            preferred_element_type=jnp.float32)
            if first:
                DW[ls, m] = value
            else:
                DW[ls, m] += value

    for m in range(3):
        weight_terms(m, group, True)
    for ll in range(2):
        for xx in range(nx):
            b = ll * nx + xx
            i = ll * tp + xx * 2 + c
            for p in range(2):
                arrived(Q.at[p, b], psend.at[p, b], precv.at[p, b])
                S[p, b] = (P[p, block(i)].astype(jnp.float32)
                           + Q[p, b].astype(jnp.float32)).astype(jnp.bfloat16)
    for k in range(1, nx):
        xx = lax.rem(x + k, nx)
        for ll in range(2):
            for p in range(2):
                send(None, S.at[p, ll * nx + xx], T.at[p, ll * nx + x], qsend.at[p, ll * nx + k],
                     qrecv.at[p, ll * nx + x], dev(xx, y, z, c))

    def relay_terms(m):
        for k in range(1, nh):
            g = lax.rem(h + k, nh) * ny + y
            arrived(G.at[m, g], gsend.at[m, g, 0], grecv.at[m, g])
            for j in range(1, ny):
                send(None, G.at[m, g], G.at[m, g], gsend.at[m, g, nh + j - 1], grecv.at[m, g],
                     dev(x, lax.rem(y + j, ny), z, c))

    relay_terms(0)
    forward_columns((1 - l) * tp + t, token_targets(True)[1:], False)
    for xx in around(nx, x):
        forward_columns(l * tp + xx * 2 + c, token_targets(False), False)
        forward_columns((1 - l) * tp + xx * 2 + c, token_targets(False), False)
    relay_terms(1)

    for ll in (1 - l, l):
        for p in range(2):
            total = S[p, ll * nx + x].astype(jnp.float32)
            for xx in around(nx, x):
                arrived(T.at[p, ll * nx + xx], qsend.at[p, 0], qrecv.at[p, ll * nx + xx])
                total += T[p, ll * nx + xx].astype(jnp.float32)
            O[p, ll] = total.astype(jnp.bfloat16)
    for p in range(2):
        send(None, O.at[p, 1 - l], T.at[p, l * nx + x], qsend.at[p, 0], qrecv.at[p, l * nx + x],
             dev(x, y, pair, c))
    for ll in range(2):
        for xx in range(nx):
            i = ll * tp + xx * 2 + 1 - c
            for dh, dy in others:
                g = lax.rem(h + dh, nh) * ny + lax.rem(y + dy, ny)
                arrived(C.at[:, g, block(i)], fsend.at[g, i, 0], frecv.at[g, i])

    for m in range(3):
        for k in range(1, nh):
            weight_terms(m, lax.rem(h + k, nh) * ny + y, False)
        for j in range(1, ny):
            g = h * ny + lax.rem(y + j, ny)
            arrived(G.at[m, g], gsend.at[m, g, 0], grecv.at[m, g])
            weight_terms(m, g, False)
        if m == 0:
            relay_terms(2)
        for k in range(1, nh):
            for j in range(1, ny):
                g = lax.rem(h + k, nh) * ny + lax.rem(y + j, ny)
                arrived(G.at[m, g], gsend.at[m, g, 0], grecv.at[m, g])
                weight_terms(m, g, False)
        DP[0, m] = DW[1 - l, m].astype(jnp.bfloat16)
        DP[1, m] = DW[l, m].astype(jnp.bfloat16)
        send(None, DP.at[0, m], terms_o.at[c, m], dsend.at[0, m], drecv.at[c, m],
             dev(x, y, pair, l))
        pl.when(c == l)(lambda m=m: pltpu.make_async_copy(
            DP.at[1, m], terms_o.at[c, m], drecv.at[c, m]).start())
        send(c != l, DP.at[1, m], terms_o.at[c, m], dsend.at[1, m], drecv.at[c, m], sibling)
    for p in range(2):
        at = (1 - l) * nx + x
        arrived(T.at[p, at], qsend.at[p, 0], qrecv.at[p, at])
        O[p, 2] = (O[p, l].astype(jnp.float32)
                   + T[p, at].astype(jnp.float32)).astype(jnp.bfloat16)
    results = [pltpu.make_async_copy(O.at[p, 2], ref, osem.at[p])
               for p, ref in enumerate((out_o, gin_o))]

    for cond, *copy in pending:
        def finish(copy=copy):
            remote(*copy).wait_send()

        if cond is None:
            finish()
        else:
            pl.when(cond)(finish)
    for copy in results:
        copy.start()
    for q in range(6):
        for zz in range(nz):
            s = zz * ny + y
            for k in range(1, ny):
                remote(slot(q, s), slot(q, s), ysend.at[q, zz, k], wrecv.at[q, s],
                       dev(x, lax.rem(y + k, ny), z, c)).wait_send()
    for cc in range(2):
        arrived(hid_o.at[cc], hsend.at[cc], hrecv.at[cc])
        for m in range(3):
            arrived(terms_o.at[cc, m], dsend.at[0, m], drecv.at[cc, m])
    for copy in results:
        copy.wait()


def finish_kernel(factor, terms, acc0, acc1, acc2, hidden, a, b, new0, new1, new2, saved, a_o, b_o):
    for m, (acc, new) in enumerate(((acc0, new0), (acc1, new1), (acc2, new2))):
        new[...] = acc[...] + factor * terms[0, m].astype(jnp.float32)

    def rest():
        half = hidden.shape[2]
        saved[:, pl.ds(0, half)] = hidden[0]
        saved[:, pl.ds(half, half)] = hidden[1]
        a_o[...] = a[...]
        b_o[...] = b[...]

    pl.when(pl.program_id(0) == 0)(rest)


def layered(x_next, x_prev, grad_out, gate_w, up_w, down_w, acc_gate, acc_up, acc_down):
    fs, tp = lax.axis_size("fs"), lax.axis_size("tp")
    ny = columns_of(fs)
    nz, nx = fs // ny, tp // 2
    rows, model = x_prev.shape
    depth, width = gate_w.shape
    half, tokens = width // 2, 2 * tp * rows
    groups, blocks = nz // 2 * ny, 2 * nx
    factor = 1.0 / math.sqrt(rows * tp * fs)
    bf, sems = jnp.bfloat16, pltpu.SemaphoreType.DMA
    out_next, grad_input, hidden, terms = pl.pallas_call(
        lambda *refs: step_kernel(nz, ny, nx, *refs),
        out_shape=[jax.ShapeDtypeStruct(s, bf) for s in (
            (rows, model), (rows, model), (2, tp * rows, half), (2, 3, half, depth))],
        in_specs=[ANY] * 6,
        out_specs=[ANY] * 4,
        scratch_shapes=[
            pltpu.VMEM((3, fs, half, depth), bf),
            pltpu.VMEM((3, tokens, model), bf),
            pltpu.VMEM((4, groups, tokens, depth), bf),
            pltpu.VMEM((3, half, tokens), jnp.float32),
            pltpu.VMEM((2, tokens, half), jnp.float32),
            pltpu.VMEM((3, groups, half, tokens), bf),
            pltpu.VMEM((2, tokens, half), bf),
            pltpu.VMEM((tokens, half), bf),
            pltpu.VMEM((2, tokens, model), bf),
            pltpu.VMEM((2, blocks, rows, model), bf),
            pltpu.VMEM((2, blocks, rows, model), bf),
            pltpu.VMEM((2, blocks, rows, model), bf),
            pltpu.VMEM((2, 3, rows, model), bf),
            pltpu.VMEM((2, 3, half, depth), jnp.float32),
            pltpu.VMEM((2, 3, half, depth), bf),
            sems((6, nz, 2)), sems((6, fs)), sems((6, nz, ny)),
            sems((3, 2 * tp, nx + 1)), sems((3, 2 * tp)),
            sems((4, groups)), sems((4, groups)),
            sems((groups, 2 * tp, nx + 1)), sems((groups, 2 * tp)),
            sems((3, groups, nz // 2 + ny)), sems((3, groups)),
            sems((2, blocks)), sems((2, blocks)), sems((2, blocks)), sems((2, blocks)),
            sems((2,)), sems((2,)), sems((2, 3)), sems((2, 3)), sems((2,)),
        ],
        compiler_params=pltpu.CompilerParams(has_side_effects=True, collective_id=0),
        name="step",
    )(gate_w.T, up_w.T, down_w, x_next, x_prev, grad_out)
    piece = half // 2
    piece_spec = pl.BlockSpec((piece, depth), lambda i: (i, 0))

    def whole(*shape):
        return pl.BlockSpec(shape, lambda i: (0,) * len(shape))

    new_gate, new_up, new_down, saved, out_next, grad_input = pl.pallas_call(
        lambda *refs: finish_kernel(factor, *refs),
        grid=(4,),
        out_shape=[jax.ShapeDtypeStruct((width, depth), jnp.float32)] * 3 + [
            jax.ShapeDtypeStruct((tp * rows, width), bf)]
        + [jax.ShapeDtypeStruct((rows, model), bf)] * 2,
        in_specs=[pl.BlockSpec((1, 3, piece, depth), lambda i: (i // 2, 0, i % 2, 0))]
        + [piece_spec] * 3 + [whole(2, tp * rows, half), whole(rows, model), whole(rows, model)],
        out_specs=[piece_spec] * 3
        + [whole(tp * rows, width), whole(rows, model), whole(rows, model)],
        name="finish",
    )(terms, acc_gate.T, acc_up.T, acc_down, hidden, out_next, grad_input)
    return (out_next, saved, grad_input, new_gate.T, new_up.T, new_down)


def layers_fit(fs, tp, rows, depth, width):
    nz = fs // columns_of(fs)
    return nz % 2 == 0 and tp % 2 == 0 and depth % 128 == 0 and width % 64 == 0 and rows % 16 == 0


def choose(*args):
    depth, width = args[3].shape
    fits = layers_fit(lax.axis_size("fs"), lax.axis_size("tp"), args[0].shape[0], depth, width)
    return (layered if fits else local)(*args)


def solution(mesh):
    in_specs = (
        P(("fs", "tp"), None),
        P(("fs", "tp"), None),
        P(("fs", "tp"), None),
        P("fs", "tp"),
        P("fs", "tp"),
        P("tp", "fs"),
        P("fs", "tp"),
        P("fs", "tp"),
        P("tp", "fs"),
    )
    out_specs = (
        P(("fs", "tp"), None),
        P("fs", "tp"),
        P(("fs", "tp"), None),
        P("fs", "tp"),
        P("fs", "tp"),
        P("tp", "fs"),
    )
    return jax.shard_map(choose, mesh=mesh, in_specs=in_specs, out_specs=out_specs, check_vma=False)
```
